32 devices in a mesh: fs: 16 (over z, y, x), tp: 2 (over core).
Axes of the slice: x: 2, y: 2, z: 4, core: 2. Of those that a mesh axis runs over, the one named last changes fastest.
Arguments:
- tokens: bfloat16 [6144, 2048], P('fs', 'tp'), may hold values from -6 to 6
- outer_gate: bfloat16 [2048, 2048], P('fs', 'tp'), may hold values from -0.125 to 0.125
- inner_gate: bfloat16 [2048, 2048], P('fs', 'tp'), may hold values from -0.125 to 0.125
- mix_value: bfloat16 [2048, 2048], P('fs', 'tp'), may hold values from -0.125 to 0.125
- mix_taps: bfloat16 [3, 2048], P(None, 'tp'), may hold values from -3 to 3
- mix_out: bfloat16 [2048, 2048], P('tp', 'fs'), may hold values from -0.1875 to 0.1875
- mix_gain: bfloat16 [2048], P('tp'), may hold values from 0.099609375 to 1.8984375
- ffn_gate: bfloat16 [2048, 3072], P('fs', 'tp'), may hold values from -0.125 to 0.125
- ffn_value: bfloat16 [2048, 3072], P('fs', 'tp'), may hold values from -0.125 to 0.125
- gate_taps: bfloat16 [3, 3072], P(None, 'tp'), may hold values from -3 to 3
- value_taps: bfloat16 [3, 3072], P(None, 'tp'), may hold values from -3 to 3
- ffn_down: bfloat16 [3072, 2048], P('tp', 'fs'), may hold values from -0.15625 to 0.15625
- ffn_gain: bfloat16 [2048], P('tp'), may hold values from 0.099609375 to 1.8984375
Outputs:
- layer_out: bfloat16 [6144, 2048], P('fs', 'tp')
The draws below stay inside these ranges and needn't reach their ends.
All inputs are finite; a program needn't handle non-finite values.
Results may differ from the reference program's by a relative error of at most 0.015.
Values may be sent and summed in bfloat16 or wider, within the bound.
A program may use at most 64 MiB of HBM per device.

```python
import jax
import jax.numpy as jnp
from jax import lax

D = 2048
F = 3072
SEQ_LEN = 128
TOKENS = 6144
N_TP = 2


def with_spikes(values, own_key, source, target, blocks, factor):
    def block_of(dim):
        return (jnp.arange(values.shape[dim]) // (values.shape[dim] // blocks)).reshape((-1,) + (1,) * (values.ndim - 1 - dim))

    one_side = jax.random.permutation(own_key, blocks)[block_of(target)]
    far = (block_of(target) + blocks // 2) % blocks
    return jnp.where((block_of(source) == one_side) | (block_of(source) == far), factor * values, values)


def shard_levels(key, shape, pieces, smallest, high):
    loudness = 1.0
    for axis_at, shards_of in pieces:
        heights = jax.random.uniform(jax.random.fold_in(jax.random.fold_in(key, 6), axis_at), (shards_of,), jnp.float32, smallest / len(pieces), high / len(pieces))
        loudness = loudness * jnp.repeat(jnp.exp(heights), shape[axis_at] // shards_of).reshape((-1,) + (1,) * (len(shape) - 1 - axis_at))
    return loudness


def noise(stream_key, extent, scale, most, pieces=(), kind=jnp.bfloat16):
    values = jax.random.normal(stream_key, extent, jnp.float32) * scale
    if len(pieces) > 0:
        values = shard_levels(stream_key, extent, pieces, -0.22, 0.18) * values
    return jnp.clip(values, min=-most, max=most).astype(kind)


def heavy_noise(stream_key, extent, deviation, bound, cuts, heavy, kind=jnp.bfloat16):
    drawn = deviation * jax.random.normal(stream_key, extent, jnp.float32)
    if cuts:
        drawn = drawn * shard_levels(stream_key, extent, cuts, -0.22, 0.18)
    return jnp.clip(with_spikes(drawn, jax.random.fold_in(stream_key, 3), *heavy), -bound, bound).astype(kind)


def setup_inputs(seed: int = 0) -> dict:
    streams_of = jax.random.split(jax.random.key(seed), 14)
    return {
        "tokens": noise(streams_of[0], (TOKENS, D), 1.0, 6.0, ((0, 16), (1, 2))),
        "outer_gate": noise(streams_of[1], (D, D), D ** -0.5, 0.125, ((0, 16), (1, 2))),
        "inner_gate": noise(streams_of[2], (D, D), D ** -0.5, 0.125, ((0, 16), (1, 2))),
        "mix_value": noise(streams_of[3], (D, D), D ** -0.5, 0.125, ((0, 16), (1, 2))),
        "mix_taps": noise(streams_of[4], (3, D), 0.577, 3.0, ((1, 2),)),
        "mix_out": heavy_noise(streams_of[5], (D, D), D ** -0.5, 0.1875, ((0, 2), (1, 16)), (0, 1, 16, 2.0)),
        "mix_gain": jnp.clip(1.0 + 0.18 * jax.random.normal(streams_of[6], (D,), jnp.float32), 0.099609375, 1.8984375).astype(jnp.bfloat16),
        "ffn_gate": noise(streams_of[7], (D, F), D ** -0.5, 0.125, ((0, 16), (1, 2))),
        "ffn_value": noise(streams_of[8], (D, F), D ** -0.5, 0.125, ((0, 16), (1, 2))),
        "gate_taps": noise(streams_of[9], (3, F), 0.577, 3.0, ((1, 2),)),
        "value_taps": noise(streams_of[10], (3, F), 0.577, 3.0, ((1, 2),)),
        "ffn_down": heavy_noise(streams_of[11], (F, D), F ** -0.5, 0.15625, ((0, 2), (1, 16)), (0, 1, 16, 2.0)),
        "ffn_gain": jnp.clip(1.0 + 0.18 * jax.random.normal(streams_of[12], (D,), jnp.float32), 0.099609375, 1.8984375).astype(jnp.bfloat16),
    }


residual_scale = 8.0 ** 0.25
norm_epsilon = 1e-05

def stored(values):
    return lax.optimization_barrier(values.astype(jnp.bfloat16)).astype(jnp.float32)

def shift_rows(values, offset):
    position = jnp.arange(values.shape[0]) % SEQ_LEN
    shifted = jnp.concatenate([jnp.zeros((offset, values.shape[1]), values.dtype), values[:-offset]], axis=0)
    return jnp.where((position >= offset)[:, None], shifted, jnp.zeros_like(shifted))

def causal_taps(values, taps):
    weights = taps.astype(jnp.float32)
    return values * weights[2] + shift_rows(values, 1) * weights[1] + shift_rows(values, 2) * weights[0]

def norm_rows(hidden, gain):
    mean = lax.optimization_barrier(jnp.mean(hidden, axis=1, keepdims=True))
    spread = lax.optimization_barrier(jnp.mean(jnp.square(hidden - mean), axis=1, keepdims=True))
    return ((hidden - mean) * lax.rsqrt(spread + norm_epsilon) * gain.astype(jnp.float32)).astype(jnp.bfloat16)

def split_sum(left, right):
    width = left.shape[1] // N_TP
    total = jnp.zeros((left.shape[0], right.shape[1]), jnp.float32)
    for index in range(N_TP):
        term = jnp.dot(left[:, index * width:(index + 1) * width], right[index * width:(index + 1) * width], preferred_element_type=jnp.float32)
        total = total + stored(term)
    return total

def reference(tokens, outer_gate, inner_gate, mix_value, mix_taps, mix_out, mix_gain, ffn_gate, ffn_value, gate_taps, value_taps, ffn_down, ffn_gain):
    outer = stored(jnp.dot(tokens, outer_gate, preferred_element_type=jnp.float32))
    inner = stored(jnp.dot(tokens, inner_gate, preferred_element_type=jnp.float32))
    values = stored(jnp.dot(tokens, mix_value, preferred_element_type=jnp.float32))
    gated = (outer * causal_taps(inner * values, mix_taps)).astype(jnp.bfloat16)
    mixer_branch = split_sum(gated, mix_out)
    first = norm_rows(residual_scale * tokens.astype(jnp.float32) + mixer_branch, mix_gain)
    gate_up = stored(jnp.dot(first, ffn_gate, preferred_element_type=jnp.float32))
    value_up = stored(jnp.dot(first, ffn_value, preferred_element_type=jnp.float32))
    hidden = (jax.nn.silu(causal_taps(gate_up, gate_taps)) * causal_taps(value_up, value_taps)).astype(jnp.bfloat16)
    ffn_branch = split_sum(hidden, ffn_down)
    return norm_rows(residual_scale * first.astype(jnp.float32) + ffn_branch, ffn_gain)
```

```python
import jax
import jax.numpy as jnp
from jax import lax
from jax.experimental import pallas as pl
from jax.experimental.pallas import tpu as pltpu
from jax.sharding import PartitionSpec as P

SEQ_LEN = 128


residual_scale = 8.0**0.25
norm_epsilon = 1e-05


def stored(values):
    return lax.optimization_barrier(values.astype(jnp.bfloat16)).astype(jnp.float32)


def shift_rows(values, offset):
    position = jnp.arange(values.shape[0]) % SEQ_LEN
    shifted = jnp.concatenate(
        [jnp.zeros((offset, values.shape[1]), values.dtype), values[:-offset]], axis=0
    )
    return jnp.where((position >= offset)[:, None], shifted, jnp.zeros_like(shifted))


def causal_taps(values, taps):
    weights = taps.astype(jnp.float32)
    return (
        values * weights[2]
        + shift_rows(values, 1) * weights[1]
        + shift_rows(values, 2) * weights[0]
    )


def fold_rows(whole, pieces):
    return tuple((jnp.dot(whole, piece, preferred_element_type=jnp.float32) for piece in pieces))


def norm_shares(prenorm, gain):
    width = prenorm.shape[1] * lax.axis_size("tp")
    row_sums = jnp.sum(prenorm, axis=1)
    row_squares = jnp.sum(prenorm * prenorm, axis=1)
    total, total_squares = lax.psum((row_sums, row_squares), "tp")
    mean = total / width
    spread = total_squares / width - mean * mean
    scaled = (prenorm - mean[:, None]) * lax.rsqrt(spread[:, None] + norm_epsilon)
    return (scaled * gain.astype(jnp.float32)).astype(jnp.bfloat16)


def plain_body(
    tokens,
    outer_gate,
    inner_gate,
    mix_value,
    mix_taps,
    mix_out,
    mix_gain,
    ffn_gate,
    ffn_value,
    gate_taps,
    value_taps,
    ffn_down,
    ffn_gain,
):
    whole_tokens = lax.all_gather(tokens, "tp", axis=1, tiled=True)
    outer, inner, values = fold_rows(
        whole_tokens,
        (
            lax.all_gather(outer_gate, "fs", axis=0, tiled=True),
            lax.all_gather(inner_gate, "fs", axis=0, tiled=True),
            lax.all_gather(mix_value, "fs", axis=0, tiled=True),
        ),
    )
    outer, inner, values = (stored(outer), stored(inner), stored(values))
    gated = (outer * causal_taps(inner * values, mix_taps)).astype(jnp.bfloat16)
    mixer_terms = jnp.dot(
        gated, lax.all_gather(mix_out, "fs", axis=1, tiled=True), preferred_element_type=jnp.float32
    )
    mixer_branch = lax.psum_scatter(
        mixer_terms.astype(jnp.bfloat16), "tp", scatter_dimension=1, tiled=True
    ).astype(jnp.float32)
    first_own = norm_shares(residual_scale * tokens.astype(jnp.float32) + mixer_branch, mix_gain)
    first_whole = lax.all_gather(first_own, "tp", axis=1, tiled=True)
    gate_up, value_up = fold_rows(
        first_whole,
        (
            lax.all_gather(ffn_gate, "fs", axis=0, tiled=True),
            lax.all_gather(ffn_value, "fs", axis=0, tiled=True),
        ),
    )
    gate_up, value_up = (stored(gate_up), stored(value_up))
    hidden = (
        jax.nn.silu(causal_taps(gate_up, gate_taps)) * causal_taps(value_up, value_taps)
    ).astype(jnp.bfloat16)
    ffn_terms = jnp.dot(
        hidden,
        lax.all_gather(ffn_down, "fs", axis=1, tiled=True),
        preferred_element_type=jnp.float32,
    )
    ffn_branch = lax.psum_scatter(
        ffn_terms.astype(jnp.bfloat16), "tp", scatter_dimension=1, tiled=True
    ).astype(jnp.float32)
    return norm_shares(residual_scale * first_own.astype(jnp.float32) + ffn_branch, ffn_gain)


PLANE = 4
LAYERS = 4
SEMAPHORES = 340
MESH = pl.DeviceIdType.MESH


def narrow(value):
    return value.astype(jnp.bfloat16)


def wide(value):
    return value.astype(jnp.float32)


def layer_kernel(
    tokens, outer_gate, inner_gate, mix_value, mix_taps, mix_out, gains, ffn_gate, ffn_value,
    gate_taps, value_taps, ffn_down,
    out,
    rows_in, up_mix, down_mix, up_ffn, down_ffn, acc, gated, hidden, parts, others, relay_x, relay_y,
    final_x, final_y, branch, first, gain_other, staged, sems,
):
    me = lax.axis_index("fs")
    core = lax.axis_index("tp")
    z, q = me // PLANE, me % PLANE
    x, y = q % 2, q // 2
    q_x, q_y, q_far = y * 2 + (1 - x), (1 - y) * 2 + x, (1 - y) * 2 + (1 - x)
    spots = (q, q_x, q_y, q_far)
    upper = z // 2
    depth = z * (1 - upper) + (3 - z) * upper

    def layer(k):
        return k + upper * (3 - 2 * k)

    near = layer(1 - depth)
    across, last = layer(2), layer(3)
    is_middle = depth == 1

    halves, half_rows, half_width = tokens.shape
    block = halves * half_rows
    quarter_rows = half_rows // 2
    depth_rows = outer_gate.shape[0]
    mix_width = up_mix.shape[2] // 3
    ffn_width = up_ffn.shape[2] // 2
    out_width = mix_out.shape[1]
    columns = down_mix.shape[2]
    slab = PLANE * depth_rows
    sequences = acc.shape[0]
    per_block = block // SEQ_LEN
    full_width = 2 * half_width

    def in_plane(spot):
        return {"fs": z * PLANE + spot}

    def at_layer(level):
        return {"fs": level * PLANE + q}

    sibling = {"tp": 1 - core}

    counter = [0]

    def claim(n=1):
        base = counter[0]
        counter[0] += n
        assert counter[0] <= SEMAPHORES
        return base

    pending = []

    def send(src, dst, send_at, recv_at, device, when=None):
        send_when(lambda: (src, dst, send_at, recv_at, device), when)

    def send_when(plan, when):
        def copy():
            src, dst, send_at, recv_at, device = plan()
            return pltpu.make_async_remote_copy(
                src_ref=src,
                dst_ref=dst,
                send_sem=sems.at[send_at],
                recv_sem=sems.at[recv_at],
                device_id=device,
                device_id_type=MESH,
            )

        pending.append((when, lambda: copy().wait_send()))
        copy().start()

    def arrive(dst, recv_at, device):
        pltpu.make_async_remote_copy(
            src_ref=dst,
            dst_ref=dst,
            send_sem=sems.at[recv_at],
            recv_sem=sems.at[recv_at],
            device_id=device,
            device_id_type=MESH,
        ).wait_recv()

    def aligned(index, step):
        return pl.multiple_of(index * step, step)

    barrier = pltpu.get_barrier_semaphore()
    for device in (in_plane(q_x), in_plane(q_y), in_plane(q_far), sibling, at_layer(near)):
        pl.semaphore_signal(barrier, inc=1, device_id=device, device_id_type=MESH)

    @pl.when(is_middle)
    def _():
        pl.semaphore_signal(barrier, inc=1, device_id=at_layer(across), device_id_type=MESH)

    pl.semaphore_wait(barrier, 5 + depth)

    def up_pieces(arrays, target):
        width = target.shape[2] // len(arrays)
        pieces = []
        for at, array in enumerate(arrays):
            def src(spot, array=array):
                return array.at[:, pl.ds(aligned(spot, width), width)]

            def dst(spot, at=at):
                return target.at[z * PLANE + spot, :, at * width : (at + 1) * width]

            pieces.append((src, dst))
        return pieces

    def down_pieces(array, target):
        width = target.shape[1]

        def src(spot):
            return array.at[pl.ds(aligned(spot, width), width), :]

        def dst(spot):
            return target.at[z, :, pl.ds(aligned(spot, out_width), out_width)]

        return [(src, dst)]

    def cut(pieces):
        recv_at = [claim(PLANE) for _ in pieces]
        local_at = [claim() for _ in pieces]
        send_at = [[claim() for _ in range(3)] for _ in pieces]

        def start_local():
            for (src, dst), at in zip(pieces, local_at):
                pltpu.make_async_copy(src(q), dst(q), sems.at[at]).start()

        def start():
            for r in (1, 2, 3):
                for (src, dst), got, sent in zip(pieces, recv_at, send_at):
                    send(src(spots[r]), dst(q), sent[r - 1], got + q, in_plane(spots[r]))

        def wait(r):
            for (src, dst), got, at in zip(pieces, recv_at, local_at):
                if r == 0:
                    pltpu.make_async_copy(src(q), dst(q), sems.at[at]).wait()
                else:
                    arrive(dst(spots[r]), got + spots[r], in_plane(spots[r]))

        return start_local, start, wait

    cut_in = cut(up_pieces((outer_gate, inner_gate, mix_value), up_mix))
    cut_out = cut(down_pieces(mix_out, down_mix))
    cut_gv = cut(up_pieces((ffn_gate, ffn_value), up_ffn))
    cut_down = cut(down_pieces(ffn_down, down_ffn))

    def z_stream(count, view):
        recv_at, near_at, across_at = claim(count), claim(count), claim(count)

        def to_near(at, when=None):
            send_when(lambda: (view(at), view(at), near_at + at, recv_at + at, at_layer(near)), when)

        def to_across(at):
            send_when(
                lambda: (view(at), view(at), across_at + at, recv_at + at, at_layer(across)), is_middle
            )

        def wait(at, level):
            arrive(view(at), recv_at + at, at_layer(level))

        return to_near, to_across, wait

    z_in = z_stream(LAYERS * PLANE, lambda at: up_mix.at[at])
    z_out = z_stream(LAYERS, lambda at: down_mix.at[at])
    z_gv = z_stream(LAYERS, lambda at: up_ffn.at[pl.ds(at * PLANE, PLANE)])
    z_down = z_stream(LAYERS, lambda at: down_ffn.at[at])

    def share(stream, at):
        stream[0](at)

        @pl.when(is_middle)
        def _():
            stream[1](at)

    def take_near(stream, at):
        stream[2](at, near)

        @pl.when(is_middle)
        def _():
            stream[1](at)

    def forward(stream, at):
        stream[2](at, across)
        stream[0](at, is_middle)

    def hand_on(stream, at):
        @pl.when(is_middle)
        def _():
            forward(stream, at)

    def take_far(stream, at):
        @pl.when(is_middle)
        def _():
            forward(stream, at)

        @pl.when(depth == 0)
        def _():
            stream[2](at, near)

    def gather(whole, top, bottom, own):
        at = {name: (claim(), claim()) for name in
              ("own", "x", "y", "far_x", "far_y", "s_x", "s_y", "s_far_x", "s_far_y")}

        def start():
            send(own, whole(q), *at["x"], in_plane(q_x))
            send(own, whole(q), *at["y"], in_plane(q_y))
            send(own, whole(q), *at["own"], sibling)

        def relay():
            arrive(whole(q_x), at["x"][1], in_plane(q_x))
            send(bottom(q_x), bottom(q_x), *at["far_y"], in_plane(q_y))
            send(whole(q_x), whole(q_x), *at["s_x"], sibling)
            arrive(whole(q_y), at["y"][1], in_plane(q_y))
            send(top(q_y), top(q_y), *at["far_x"], in_plane(q_x))
            send(whole(q_y), whole(q_y), *at["s_y"], sibling)

        def relay_far():
            arrive(bottom(q_far), at["far_y"][1], in_plane(q_y))
            send(bottom(q_far), bottom(q_far), *at["s_far_y"], sibling)
            arrive(top(q_far), at["far_x"][1], in_plane(q_x))
            send(top(q_far), top(q_far), *at["s_far_x"], sibling)

        def finish(other_whole, other_top, other_bottom):
            arrive(other_whole(q), at["own"][1], sibling)
            arrive(other_whole(q_x), at["s_x"][1], sibling)
            arrive(other_whole(q_y), at["s_y"][1], sibling)
            arrive(other_bottom(q_far), at["s_far_y"][1], sibling)
            arrive(other_top(q_far), at["s_far_x"][1], sibling)

        return start, relay, relay_far, finish

    def token_views(side):
        cols = pl.ds(aligned(side, half_width), half_width)
        return (
            lambda spot: rows_in.at[spot, :, :, cols],
            lambda spot: rows_in.at[spot, 0, :, cols],
            lambda spot: rows_in.at[spot, 1, :, cols],
        )

    def first_views(side):
        return (
            lambda spot: first.at[spot, side],
            lambda spot: first.at[spot, side, 0:quarter_rows],
            lambda spot: first.at[spot, side, quarter_rows:half_rows],
        )

    tokens_whole, tokens_top, tokens_bottom = token_views(core)
    token_gather = gather(tokens_whole, tokens_top, tokens_bottom, tokens)
    first_gather = gather(*first_views(core), first.at[q, core])

    def project(source, weights, level, levels, fresh):
        width = weights.shape[2]
        cols = pl.ds(aligned(level, slab), levels * slab)
        block_rows = pl.ds(level * PLANE, levels * PLANE)

        @pl.loop(0, PLANE)
        def _(spot):
            left = source[spot, :, :, cols].reshape(block, levels * slab)
            right = weights[block_rows].reshape(levels * slab, width)
            result = jnp.dot(left, right, preferred_element_type=jnp.float32)
            result = result.reshape(per_block, SEQ_LEN, width)
            where = pl.ds(spot * per_block, per_block)
            if fresh:
                acc[where, :, 0:width] = result
            else:
                acc[where, :, 0:width] += result

    def tapped(values, taps):
        row = lax.broadcasted_iota(jnp.int32, values.shape, 0)
        one = jnp.where(row >= 1, pltpu.roll(values, 1, 0), 0.0)
        two = jnp.where(row >= 2, pltpu.roll(values, 2, 0), 0.0)
        return values * taps[2:3] + one * taps[1:2] + two * taps[0:1]

    LANES = 128

    def own_taps(ref, width, col):
        return wide(ref[:, pl.ds(pl.multiple_of(q * width + col, LANES), LANES)])

    def mix():
        @pl.loop(0, sequences)
        def _(seq):
            for col in range(0, mix_width, LANES):
                def column(at):
                    return wide(narrow(acc[seq, :, at * mix_width + col : at * mix_width + col + LANES]))

                outer, inner, values = column(0), column(1), column(2)
                swept = tapped(inner * values, own_taps(mix_taps, mix_width, col))
                gated[seq, :, col : col + LANES] = narrow(outer * swept)

    def activate():
        @pl.loop(0, sequences)
        def _(seq):
            for col in range(0, ffn_width, LANES):
                def column(at):
                    return wide(narrow(acc[seq, :, at * ffn_width + col : at * ffn_width + col + LANES]))

                gate = tapped(column(0), own_taps(gate_taps, ffn_width, col))
                value = tapped(column(1), own_taps(value_taps, ffn_width, col))
                hidden[seq, :, col : col + LANES] = narrow(gate / (1.0 + jnp.exp(-gate)) * value)

    CHUNK = 32

    def chunks(count, body):
        @pl.loop(0, count // CHUNK)
        def _(i):
            body(pl.ds(aligned(i, CHUNK), CHUNK))

    def reduction(phase, source, weights, stream):
        levels = (depth, 1 - depth, 2, 3)
        at = [{name: (claim(), claim()) for name in
               ("sib", "far_x", "far_y", "x_top", "y_bottom", "x_bottom", "y_top")} for _ in range(LAYERS)]
        top, bottom = slice(0, quarter_rows), slice(quarter_rows, half_rows)

        def terms(step):
            level = layer(levels[step])
            if step == 1:
                take_near(stream, level)
            if step > 1:
                take_far(stream, level)

            @pl.loop(0, PLANE)
            def _(spot):
                left = source[pl.ds(spot * per_block, per_block)].reshape(block, source.shape[2])
                result = narrow(jnp.dot(left, weights[level], preferred_element_type=jnp.float32))
                parts[phase, step, spot] = result.reshape(2, half_rows, columns)

            send(parts.at[phase, step, :, 1 - core], others.at[phase, step], *at[step]["sib"], sibling)

        def join(step):
            arrive(others.at[phase, step], at[step]["sib"][1], sibling)

            def add(spot):
                def body(rows):
                    parts[phase, step, spot, core, rows] = narrow(
                        wide(parts[phase, step, spot, core, rows]) + wide(others[phase, step, spot, rows])
                    )
                chunks(half_rows, body)

            names = at[step]
            add(q_far)
            mine = parts.at[phase, step]
            send(mine.at[q_far, core, top], relay_x.at[phase, step], *names["far_x"], in_plane(q_x))
            send(mine.at[q_far, core, bottom], relay_y.at[phase, step], *names["far_y"], in_plane(q_y))
            add(q_x)
            send(mine.at[q_x, core, top], final_x.at[phase, step, top], *names["x_top"], in_plane(q_x))
            add(q_y)
            send(mine.at[q_y, core, bottom], final_y.at[phase, step, bottom], *names["y_bottom"], in_plane(q_y))

        def pass_on(step):
            names = at[step]
            mine = parts.at[phase, step]

            def add(spot, offset, arrived):
                def body(rows):
                    to = pl.ds(pl.multiple_of(rows.start + offset, CHUNK), CHUNK)
                    parts[phase, step, spot, core, to] = narrow(
                        wide(parts[phase, step, spot, core, to]) + wide(arrived[phase, step, rows])
                    )
                chunks(quarter_rows, body)

            arrive(relay_x.at[phase, step], names["far_x"][1], in_plane(q_x))
            add(q_y, 0, relay_x)
            send(mine.at[q_y, core, top], final_y.at[phase, step, top], *names["y_top"], in_plane(q_y))
            arrive(relay_y.at[phase, step], names["far_y"][1], in_plane(q_y))
            add(q_x, quarter_rows, relay_y)
            send(mine.at[q_x, core, bottom], final_x.at[phase, step, bottom], *names["x_bottom"], in_plane(q_x))

        def total(step):
            names = at[step]
            level = layer(levels[step])
            arrive(final_x.at[phase, step, top], names["x_top"][1], in_plane(q_x))
            arrive(final_y.at[phase, step, bottom], names["y_bottom"][1], in_plane(q_y))
            arrive(final_x.at[phase, step, bottom], names["x_bottom"][1], in_plane(q_x))
            arrive(final_y.at[phase, step, top], names["y_top"][1], in_plane(q_y))

            def body(rows):
                branch[level, rows] = (
                    wide(parts[phase, step, q, core, rows])
                    + wide(others[phase, step, q, rows])
                    + wide(final_x[phase, step, rows])
                    + wide(final_y[phase, step, rows])
                )
            chunks(half_rows, body)

        terms(0)
        join(0)
        terms(1)
        pass_on(0)
        join(1)
        terms(2)
        pass_on(1)
        total(0)
        join(2)
        terms(3)
        pass_on(2)
        total(1)
        join(3)
        pass_on(3)
        total(2)
        total(3)

    def norm(residual, gain_row, store):
        rows_at = 16

        @pl.loop(0, half_rows // rows_at)
        def _(i):
            rows = pl.ds(aligned(i, rows_at), rows_at)
            pieces = []
            for level in range(LAYERS):
                cols = slice(level * columns, (level + 1) * columns)
                pieces.append(residual_scale * wide(residual[q, core, rows, cols]) + branch[level, rows])
            mean = sum(jnp.sum(piece, axis=1, keepdims=True) for piece in pieces) / full_width
            spread = sum(jnp.sum(jnp.square(piece - mean), axis=1, keepdims=True) for piece in pieces) / full_width
            scale = lax.rsqrt(spread + norm_epsilon)
            for level, piece in enumerate(pieces):
                side = level // 2
                inside = slice((level % 2) * columns, (level % 2 + 1) * columns)
                gain = jnp.where(
                    core == side,
                    gains[gain_row : gain_row + 1, inside],
                    gain_other[gain_row : gain_row + 1, inside],
                )
                store(level, rows, narrow((piece - mean) * scale * gain))

    for group in (cut_in, cut_out, cut_gv, cut_down):
        group[0]()
    own_local = pltpu.make_async_copy(tokens, tokens_whole(q), sems.at[claim()])
    own_local.start()
    cut_in[1]()
    token_gather[0]()
    gain_at = (claim(), claim())
    send(gains, gain_other, *gain_at, sibling)
    cut_out[1]()
    for r in range(PLANE):
        cut_in[2](r)
        share(z_in, z * PLANE + spots[r])
    for j in range(PLANE):
        hand_on(z_in, across * PLANE + spots[j])
        take_near(z_in, near * PLANE + spots[j])
    own_local.wait()
    token_gather[1]()
    cut_gv[1]()
    cut_down[1]()
    for j in range(PLANE):
        hand_on(z_in, last * PLANE + spots[j])
    token_gather[2]()
    for r in range(PLANE):
        cut_out[2](r)
    share(z_out, z)
    token_gather[3](*token_views(1 - core))
    project(rows_in, up_mix, upper * 2, 2, True)
    for r in range(PLANE):
        cut_gv[2](r)
    share(z_gv, z)
    for r in range(PLANE):
        cut_down[2](r)
    share(z_down, z)
    for level in (across, last):
        @pl.when(depth == 0)
        def _():
            for spot in spots:
                z_in[2](level * PLANE + spot, near)
        project(rows_in, up_mix, level, 1, False)
    mix()
    reduction(0, gated, down_mix, z_out)
    arrive(gain_other, gain_at[1], sibling)

    def store_first(level, rows, value):
        first[q, core, rows, level * columns : (level + 1) * columns] = value

    norm(rows_in, 0, store_first)
    first_gather[0]()
    take_near(z_gv, near)

    hand_on(z_gv, across)
    first_gather[1]()
    hand_on(z_gv, last)
    first_gather[2]()
    first_gather[3](*first_views(1 - core))
    project(first, up_ffn, upper * 2, 2, True)
    for level in (across, last):
        @pl.when(depth == 0)
        def _():
            z_gv[2](level, near)
        project(first, up_ffn, level, 1, False)
    activate()
    reduction(1, hidden, down_ffn, z_down)

    def store_out(level, rows, value):
        staged[level // 2, rows, (level % 2) * columns : (level % 2 + 1) * columns] = value

    norm(first, 1, store_out)
    out_at = (claim(), claim())
    send(staged.at[1 - core], out.at[core], *out_at, sibling)
    keep = pltpu.make_async_copy(staged.at[core], out.at[core], sems.at[claim()])
    keep.start()
    keep.wait()
    arrive(out.at[1 - core], out_at[1], sibling)
    always = [wait for when, wait in pending if when is None]
    middle = [wait for when, wait in pending if when is not None]
    for wait in always:
        wait()

    @pl.when(is_middle)
    def _():
        for wait in middle:
            wait()


def kernel_body(
    tokens, outer_gate, inner_gate, mix_value, mix_taps, mix_out, mix_gain, ffn_gate, ffn_value,
    gate_taps, value_taps, ffn_down, ffn_gain,
):
    block, half_width = tokens.shape
    half_rows = block // 2
    width = 2 * half_width
    depth_rows = outer_gate.shape[0]
    mix_width = outer_gate.shape[1] // PLANE
    ffn_width = ffn_gate.shape[1] // PLANE
    columns = PLANE * mix_out.shape[1]
    blocks = PLANE * LAYERS
    sequences = PLANE * block // SEQ_LEN
    widest = max(3 * mix_width, 2 * ffn_width)
    half = jnp.bfloat16
    vmem, anywhere = pl.BlockSpec(memory_space=pltpu.VMEM), pl.BlockSpec(memory_space=pl.ANY)
    gains = wide(jnp.stack([mix_gain, ffn_gain]))
    result = pl.pallas_call(
        layer_kernel,
        out_shape=jax.ShapeDtypeStruct((2, half_rows, half_width), half),
        in_specs=[
            anywhere, anywhere, anywhere, anywhere, vmem, anywhere, vmem, anywhere, anywhere,
            vmem, vmem, anywhere,
        ],
        out_specs=anywhere,
        scratch_shapes=[
            pltpu.VMEM((PLANE, 2, half_rows, width), half),
            pltpu.VMEM((blocks, depth_rows, 3 * mix_width), half),
            pltpu.VMEM((LAYERS, mix_width, columns), half),
            pltpu.VMEM((blocks, depth_rows, 2 * ffn_width), half),
            pltpu.VMEM((LAYERS, ffn_width, columns), half),
            pltpu.VMEM((sequences, SEQ_LEN, widest), jnp.float32),
            pltpu.VMEM((sequences, SEQ_LEN, mix_width), half),
            pltpu.VMEM((sequences, SEQ_LEN, ffn_width), half),
            pltpu.VMEM((2, LAYERS, PLANE, 2, half_rows, columns), half),
            pltpu.VMEM((2, LAYERS, PLANE, half_rows, columns), half),
            pltpu.VMEM((2, LAYERS, half_rows // 2, columns), half),
            pltpu.VMEM((2, LAYERS, half_rows // 2, columns), half),
            pltpu.VMEM((2, LAYERS, half_rows, columns), half),
            pltpu.VMEM((2, LAYERS, half_rows, columns), half),
            pltpu.VMEM((LAYERS, half_rows, columns), jnp.float32),
            pltpu.VMEM((PLANE, 2, half_rows, width), half),
            pltpu.VMEM((2, half_width), jnp.float32),
            pltpu.VMEM((2, half_rows, half_width), half),
            pltpu.SemaphoreType.DMA((SEMAPHORES,)),
        ],
        compiler_params=pltpu.CompilerParams(
            collective_id=0, has_side_effects=True, vmem_limit_bytes=67043328
        ),
    )(
        tokens.reshape(2, half_rows, half_width), outer_gate, inner_gate, mix_value, mix_taps, mix_out,
        gains, ffn_gate, ffn_value, gate_taps, value_taps, ffn_down,
    )
    return result.reshape(block, half_width)


def solution(mesh):
    folds = mesh.shape["fs"] == PLANE * LAYERS and mesh.shape["tp"] == 2
    body = kernel_body if folds else plain_body
    placed = (
        P("fs", "tp"),
        P("fs", "tp"),
        P("fs", "tp"),
        P("fs", "tp"),
        P(None, "tp"),
        P("tp", "fs"),
        P("tp"),
        P("fs", "tp"),
        P("fs", "tp"),
        P(None, "tp"),
        P(None, "tp"),
        P("tp", "fs"),
        P("tp"),
    )
    return jax.shard_map(body, mesh=mesh, in_specs=placed, out_specs=P("fs", "tp"), check_vma=False)
```
